32 devices in a mesh: fs: 8 (over z, y), tp: 4 (over x, core).
Axes of the slice: x: 2, y: 2, z: 4, core: 2. Of those that a mesh axis runs over, the one named last changes fastest.
Arguments:
- tokens: bfloat16 [8192, 2048], P('fs', 'tp'), may hold values from -40 to 40
- first_gain: float32 [2048], replicated, may hold values from 0.1 to 1.9
- first_gate: bfloat16 [2048, 6144], P('fs', 'tp'), may hold values from -0.125 to 0.125
- first_upward: bfloat16 [2048, 6144], P('fs', 'tp'), may hold values from -0.125 to 0.125
- first_down: bfloat16 [6144, 2048], P('tp', 'fs'), may hold values from -0.078125 to 0.078125
- mix_gain: float32 [2048], replicated, may hold values from 0.1 to 1.9
- mix_input: bfloat16 [2048, 1024], P('fs', 'tp'), may hold values from -0.125 to 0.125
- pool_weight: bfloat16 [8, 128, 128], replicated, may hold values from -0.5 to 0.5
- pool_scale: float32 [1024], replicated, may hold values from 0.1 to 1.9
- mix_output: bfloat16 [1024, 2048], P('tp', 'fs'), may hold values from -0.1875 to 0.1875
- second_gain: float32 [2048], replicated, may hold values from 0.1 to 1.9
- second_gate: bfloat16 [2048, 6144], P('fs', 'tp'), may hold values from -0.125 to 0.125
- second_upward: bfloat16 [2048, 6144], P('fs', 'tp'), may hold values from -0.125 to 0.125
- second_down: bfloat16 [6144, 2048], P('tp', 'fs'), may hold values from -0.078125 to 0.078125
Outputs:
- layer_out: bfloat16 [8192, 2048], P('fs', 'tp')
The draws below stay inside these ranges and needn't reach their ends.
All inputs are finite; a program needn't handle non-finite values.
Results may differ from the reference program's by a relative error of at most 0.01.
Values may be sent and summed in bfloat16 or wider, within the bound.
A program may use at most 128 MiB of HBM per device.

```python
import math
import jax
import jax.numpy as jnp
from jax import lax

D = 2048
FF = 6144
GROUPS = 8
GROUP_DIM = 128
TOK_DEV = 1024
POOL_WIDTH = 1024
TOKENS = 8192
N_FS = 8
N_TP = 4


def draw_tokens(key, part):
    keys = jax.random.split(jax.random.fold_in(key, 11), 3)
    base = jax.random.normal(keys[0], (TOKENS, D), jnp.float32)
    base = jnp.clip(base, -4.0, 4.0)
    row_scale = jnp.exp(jax.random.uniform(keys[1], (TOKENS, 1), jnp.float32, math.log(0.5), math.log(5.0)))
    col_scale = jnp.exp(jax.random.uniform(keys[2], (1, D), jnp.float32, math.log(0.5), math.log(2.0)))
    return (base * row_scale * col_scale).astype(jnp.bfloat16)


def shard_levels(stream_key, shape, shards, low, high):
    gain, own = 1.0, jax.random.fold_in(stream_key, 6)
    for axis_at, blocks in shards:
        draws = jnp.exp(jax.random.uniform(jax.random.fold_in(own, axis_at), (blocks,), jnp.float32, low / len(shards), high / len(shards)))
        gain = gain * jnp.repeat(draws, shape[axis_at] // blocks).reshape([-1 if axis == axis_at else 1 for axis in range(len(shape))])
    return gain


def normal_values(key, dims, scale, limit, shards=(), kind=jnp.bfloat16):
    values = scale * jax.random.normal(key, dims, jnp.float32)
    if shards:
        values = values * shard_levels(key, dims, shards, -0.22, 0.18)
    return jnp.clip(values, -limit, limit).astype(kind)


def setup_inputs(seed: int = 0) -> dict:
    streams_of = jax.random.split(jax.random.key(seed), 15)
    tokens = draw_tokens(jax.random.fold_in(streams_of[14], 71), 0)
    first_gain = jnp.clip(1.0 + 0.18 * jax.random.normal(streams_of[1], (D,), jnp.float32), 0.1, 1.9)
    first_gate = normal_values(streams_of[2], (D, FF), D ** -0.5, 0.125, ((0, 8), (1, 4)))
    first_upward = normal_values(streams_of[3], (D, FF), D ** -0.5, 0.125, ((0, 8), (1, 4)))
    first_down = normal_values(streams_of[4], (FF, D), FF ** -0.5, 0.078125, ((0, 4), (1, 8)))
    mix_gain = jnp.clip(1.0 + 0.18 * jax.random.normal(streams_of[5], (D,), jnp.float32), 0.1, 1.9)
    mix_input = normal_values(streams_of[6], (D, POOL_WIDTH), D ** -0.5, 0.125, ((0, 8), (1, 4)))
    pool_weight = normal_values(streams_of[7], (GROUPS, GROUP_DIM, GROUP_DIM), GROUP_DIM ** -0.5, 0.5)
    pool_scale = jnp.clip(1.0 + 0.18 * jax.random.normal(streams_of[8], (POOL_WIDTH,), jnp.float32), 0.1, 1.9)
    mix_output = normal_values(streams_of[9], (POOL_WIDTH, D), POOL_WIDTH ** -0.5, 0.1875, ((0, 4), (1, 8)))
    second_gain = jnp.clip(1.0 + 0.18 * jax.random.normal(streams_of[10], (D,), jnp.float32), 0.1, 1.9)
    second_gate = normal_values(streams_of[11], (D, FF), D ** -0.5, 0.125, ((0, 8), (1, 4)))
    second_upward = normal_values(streams_of[12], (D, FF), D ** -0.5, 0.125, ((0, 8), (1, 4)))
    second_down = normal_values(streams_of[13], (FF, D), FF ** -0.5, 0.078125, ((0, 4), (1, 8)))
    return {"tokens": tokens, "first_gain": first_gain, "first_gate": first_gate, "first_upward": first_upward, "first_down": first_down, "mix_gain": mix_gain, "mix_input": mix_input, "pool_weight": pool_weight, "pool_scale": pool_scale, "mix_output": mix_output, "second_gain": second_gain, "second_gate": second_gate, "second_upward": second_upward, "second_down": second_down}


EPSILON = 1e-06
REACH = 15

def normalize(values, weight_gain):
    wide = values.astype(jnp.float32)
    factor = lax.rsqrt(lax.optimization_barrier(jnp.mean(wide * wide, axis=-1, keepdims=True)) + EPSILON)
    return (wide * factor * weight_gain).astype(jnp.bfloat16)

def block_sum(left, right):
    width = left.shape[1] // N_TP
    summed = jnp.zeros((left.shape[0], right.shape[1]), jnp.float32)
    for block in range(N_TP):
        piece = jnp.dot(left[:, block * width:(block + 1) * width], right[block * width:(block + 1) * width], preferred_element_type=jnp.float32)
        summed = summed + lax.optimization_barrier(piece.astype(jnp.bfloat16)).astype(jnp.float32)
    return summed

def feed_forward(values, weight_gain, gate_weight, upward_weight, down_weight):
    normed = normalize(values, weight_gain)
    gated = jnp.dot(normed, gate_weight, preferred_element_type=jnp.float32)
    upward = jnp.dot(normed, upward_weight, preferred_element_type=jnp.float32)
    hidden = (jax.nn.silu(gated) * upward).astype(jnp.bfloat16)
    summed = block_sum(hidden, down_weight)
    return (values.astype(jnp.float32) + 0.5 * summed).astype(jnp.bfloat16)

def pool_mixer(values, mix_gain, mix_input, pool_weight, pool_scale, mix_output):
    normed = normalize(values, mix_gain)
    pool_in = jnp.dot(normed, mix_input, preferred_element_type=jnp.float32).astype(jnp.bfloat16)
    width = pool_in.shape[1]
    sequences = pool_in.reshape(N_FS, TOK_DEV, width).astype(jnp.float32)
    padded = jnp.pad(sequences, ((0, 0), (REACH, 0), (0, 0)))
    windows = jnp.left_shift(2, jnp.arange(GROUPS, dtype=jnp.int32) % 4)
    window_cols = jnp.repeat(windows, GROUP_DIM)[None, None, :]
    summed = jnp.zeros(sequences.shape, jnp.float32)
    for offset in range(REACH + 1):
        shifted = padded[:, REACH - offset:REACH - offset + TOK_DEV]
        summed = summed + jnp.where(offset < window_cols, shifted, 0.0)
    positions = jnp.arange(TOK_DEV, dtype=jnp.int32)
    counts = jnp.minimum(positions[None, :, None] + 1, window_cols).astype(jnp.float32)
    pooled = (summed / counts - sequences).astype(jnp.bfloat16).reshape(TOKENS, GROUPS, GROUP_DIM)
    mapped = jnp.einsum('tgc,gcd->tgd', pooled.astype(jnp.float32), pool_weight.astype(jnp.float32))
    mapped = (mapped.reshape(TOKENS, width) * pool_scale).astype(jnp.bfloat16)
    mixer = block_sum(mapped, mix_output)
    return (values.astype(jnp.float32) + mixer).astype(jnp.bfloat16)

def reference(tokens, first_gain, first_gate, first_upward, first_down, mix_gain, mix_input, pool_weight, pool_scale, mix_output, second_gain, second_gate, second_upward, second_down):
    first_out = feed_forward(tokens, first_gain, first_gate, first_upward, first_down)
    mid_out = pool_mixer(first_out, mix_gain, mix_input, pool_weight, pool_scale, mix_output)
    return feed_forward(mid_out, second_gain, second_gate, second_upward, second_down)
```

```python
import jax
import jax.numpy as jnp
from jax import lax
from jax.sharding import PartitionSpec as P


GROUP_DIM = 128


EPSILON = 1e-06
REACH = 15
PAIR = 2


def shifted(value, axis, steps):
    count = lax.axis_size(axis)
    initial, last = (max(0, -steps), min(count, count - steps))
    return lax.ppermute(value, axis, [(source, source + steps) for source in range(initial, last)])


def normalize(values, weight_gain):
    wide = values.astype(jnp.float32)
    factor = lax.rsqrt(jnp.mean(wide * wide, axis=-1, keepdims=True) + EPSILON)
    return (wide * factor * weight_gain).astype(jnp.bfloat16)


def swap(value, axis, mask):
    count = lax.axis_size(axis)
    return lax.ppermute(value, axis, [(source, source ^ mask) for source in range(count)])


def from_core(value):
    return swap(value, "tp", 1)


def from_chip(value, steps):
    count = lax.axis_size("tp")
    return lax.ppermute(
        value, "tp", [(source, (source + steps * PAIR) % count) for source in range(count)]
    )


def from_mate(value):
    return swap(value, "fs", PAIR)


def from_lane(value):
    return swap(value, "fs", 1)


def fetch_halves(half):
    count = lax.axis_size("fs")
    lines = count // PAIR
    me = lax.axis_index("fs")
    line, lane = me // PAIR, me % PAIR
    own, other = half(line % PAIR), half(1 - line % PAIR)
    blocks = {0: own}
    for steps in sorted(range(1, lines), reverse=True):
        blocks[steps] = swap(other if steps % 2 else own, "fs", steps * PAIR)
    found = []
    for steps, block in blocks.items():
        partner = from_lane(block)
        at = (line ^ steps) * PAIR
        found += [(block, at + lane), (partner, at + 1 - lane)]
    return found


def join(found, axis, place=lambda at: at):
    first = found[0][0]
    step = first.shape[axis]
    shape = list(first.shape)
    shape[axis] = step * len(found)
    full = jnp.zeros(shape, first.dtype)
    for block, at in found:
        start = [0] * len(shape)
        start[axis] = place(at) * step
        full = lax.dynamic_update_slice(full, block, start)
    return full


def fetch_pair(gate, upward):
    width = gate.shape[1] // PAIR

    def half(parity):
        parts = [lax.dynamic_slice_in_dim(w, parity * width, width, 1) for w in (gate, upward)]
        return jnp.concatenate(parts, 1)

    found = fetch_halves(half)
    return [
        [(block[:, which * width : (which + 1) * width], at) for block, at in found]
        for which in range(2)
    ]


def fetch_down(down):
    depth = down.shape[0] // PAIR
    return fetch_halves(lambda parity: lax.dynamic_slice_in_dim(down, parity * depth, depth, 0))


def fetch_mixer(mix_input, mix_output):
    both = jnp.concatenate([mix_input, mix_output.T], 1)
    count = lax.axis_size("fs")
    lines = count // PAIR
    me = lax.axis_index("fs")
    line, lane = me // PAIR, me % PAIR
    found = [(both, line)]
    for steps in sorted(range(1, lines), reverse=True):
        found.append((swap(both, "fs", steps * PAIR), line ^ steps))
    rows = join([(block[None], at) for block, at in found], 0)
    partner = from_lane(rows)
    lanes = jnp.stack([rows, partner], 1)
    lanes = jnp.where(lane == 0, lanes, lanes[:, ::-1])
    rows = lanes.reshape(count * both.shape[0], both.shape[1])
    return [gather_tp(rows)]


def gather_tp(value):
    count = lax.axis_size("tp")
    chips = count // PAIR
    me = lax.axis_index("tp")
    chip, core = me // PAIR, me % PAIR
    found = []
    for steps in range(chips):
        if steps:
            block = from_chip(value, steps)
        else:
            block = value
        partner = from_core(block)
        place = (chip - steps + chips) % chips * PAIR
        found += [(block, place + core), (partner, place + 1 - core)]
    return found


def wide(value):
    return value.astype(jnp.float32)


def narrow(value):
    return value.astype(jnp.bfloat16)


def hidden_units(rows, weight_gain, gate, upward):
    normed = normalize(rows, weight_gain)
    gated = jnp.dot(normed, join(gate, 0), preferred_element_type=jnp.float32)
    raised = jnp.dot(normed, join(upward, 0), preferred_element_type=jnp.float32)
    return narrow(jax.nn.silu(gated) * raised)


def send_x(values):
    chips = values.shape[0]
    chip = lax.axis_index("tp") // PAIR
    total = wide(lax.dynamic_index_in_dim(values, chip, 0, keepdims=False))
    for steps in range(1, chips):
        part = lax.dynamic_index_in_dim(values, (chip + steps) % chips, 0, keepdims=False)
        total = total + wide(from_chip(part, steps))
    return total


def scatter(sums):
    half = sums.shape[2] // 2
    one, two = sums[:, :, :half], sums[:, :, half:]
    first = narrow(send_x(jnp.swapaxes(one, 0, 1)))
    arrived = from_mate(two[1])
    second = send_x(narrow(wide(two[0]) + wide(arrived)))
    arrived = from_mate(first[1])
    return jnp.concatenate([wide(first[0]) + wide(arrived), second], 0)


def pool_groups(extended, positions, pool_weight, pool_scale):
    row_count = positions.shape[0]
    group_count = extended.shape[1] // GROUP_DIM
    group_ids = jnp.arange(group_count, dtype=jnp.int32)
    windows = jnp.left_shift(2, group_ids % 4)
    window_cols = jnp.repeat(windows, GROUP_DIM)[None, :]
    values = wide(extended)
    summed = jnp.zeros((row_count, values.shape[1]), jnp.float32)
    for offset in range(REACH + 1):
        moved = values[REACH - offset : REACH - offset + row_count]
        summed = summed + jnp.where(offset < window_cols, moved, 0.0)
    counts = jnp.minimum(positions[:, None] + 1, window_cols).astype(jnp.float32)
    pooled = narrow(summed / counts - values[REACH:])
    mapped = jnp.einsum(
        "tgc,gcd->tgd",
        pooled.reshape(row_count, group_count, GROUP_DIM),
        pool_weight,
        preferred_element_type=jnp.float32,
    )
    return narrow(mapped.reshape(row_count, group_count * GROUP_DIM) * pool_scale)


def per_device(
    tokens,
    first_gain,
    first_gate,
    first_upward,
    first_down,
    mix_gain,
    mix_input,
    pool_weight,
    pool_scale,
    mix_output,
    second_gain,
    second_gate,
    second_upward,
    second_down,
):
    tp = lax.axis_size("tp")
    chips = tp // PAIR
    me = lax.axis_index("tp")
    core = me % PAIR
    row_count, width = tokens.shape
    run = row_count // tp
    depth = width * tp

    mate_tokens = from_mate(tokens)
    own_rows = join(gather_tp(tokens), 1)
    mate_rows = join(gather_tp(mate_tokens), 1)
    rows = jnp.concatenate([own_rows, mate_rows], 0)

    gate_1, upward_1 = fetch_pair(first_gate, first_upward)
    down_1 = fetch_down(first_down)
    gate_2, upward_2 = fetch_pair(second_gate, second_upward)
    down_2 = fetch_down(second_down)
    (mixer,) = fetch_mixer(mix_input, mix_output)

    hidden = hidden_units(rows, first_gain, gate_1, upward_1)
    runs = hidden.reshape(2, chips, PAIR, run, hidden.shape[1])
    full_down = join(down_1, 1)

    def down_rows(which):
        picked = lax.dynamic_index_in_dim(runs, which, 2, keepdims=False)
        parts = jnp.dot(
            picked.reshape(-1, hidden.shape[1]), full_down, preferred_element_type=jnp.float32
        )
        return parts.reshape(2, chips, run, depth)

    arrived = from_core(narrow(down_rows(1 - core)))
    sums = narrow(down_rows(core) + wide(arrived))
    left = scatter_cols(sums)
    own_run = lax.dynamic_slice_in_dim(own_rows, me * run, run, 0)
    first_out = narrow(wide(own_run) + 0.5 * left)

    normed = normalize(first_out, mix_gain)
    channels = mix_input.shape[1]
    mixer_full = join(mixer, 1).reshape(depth, tp, 2, channels)
    full_input = mixer_full[:, :, 0].reshape(depth, tp * channels)
    full_output = mixer_full[:, :, 1].reshape(depth, tp * channels)
    pool_in = narrow(jnp.dot(normed, full_input, preferred_element_type=jnp.float32))
    prior = shifted(pool_in[run - REACH :], "tp", 1)
    extended = jnp.concatenate([prior, pool_in], 0)
    positions = me * run + jnp.arange(run, dtype=jnp.int32)
    mapped = pool_groups(extended, positions, pool_weight, pool_scale)
    mixed = lax.dot_general(
        mapped, full_output, (((1,), (1,)), ((), ())), preferred_element_type=jnp.float32
    )
    mid_run = narrow(wide(first_out) + mixed)

    mate_run = from_mate(mid_run)
    own_mid = join(gather_tp(mid_run), 0)
    mate_mid = join(gather_tp(mate_run), 0)
    rows = jnp.concatenate([own_mid, mate_mid], 0)
    hidden = hidden_units(rows, second_gain, gate_2, upward_2)
    ratio = lax.axis_size("fs") // tp

    def place(at):
        target, piece = at // ratio, at % ratio
        away = jnp.where(target % PAIR == core, 1, 0)
        return (away * chips + target // PAIR) * ratio + piece

    full_down = join(down_2, 1, place)
    half = depth // 2

    def down_cols(which):
        parts = jnp.dot(
            hidden,
            full_down[:, which * half : (which + 1) * half],
            preferred_element_type=jnp.float32,
        )
        return parts

    arrived = from_core(narrow(down_cols(0)))
    sums = narrow(down_cols(1) + wide(arrived))
    sums = jnp.stack([sums[:, c * width : (c + 1) * width] for c in range(chips)])
    sums = jnp.swapaxes(sums.reshape(chips, 2, row_count, width), 0, 1)
    summed = scatter(sums)
    own_cols = lax.dynamic_slice_in_dim(own_mid, me * width, width, 1)
    return narrow(wide(own_cols) + 0.5 * summed)


def scatter_cols(sums):
    half = sums.shape[3] // 2
    one, two = sums[..., :half], sums[..., half:]
    first = narrow(send_x(jnp.swapaxes(one, 0, 1)))
    arrived = from_mate(two[1])
    second = send_x(narrow(wide(two[0]) + wide(arrived)))
    arrived = from_mate(first[1])
    return jnp.concatenate([wide(first[0]) + wide(arrived), second], 1)


def solution(mesh):
    in_specs = (
        P("fs", "tp"),
        P(),
        P("fs", "tp"),
        P("fs", "tp"),
        P("tp", "fs"),
        P(),
        P("fs", "tp"),
        P(),
        P(),
        P("tp", "fs"),
        P(),
        P("fs", "tp"),
        P("fs", "tp"),
        P("tp", "fs"),
    )
    out_specs = P("fs", "tp")
    return jax.shard_map(
        per_device, mesh=mesh, in_specs=in_specs, out_specs=out_specs, check_vma=False
    )
```

```python
import jax
import jax.numpy as jnp
from jax import lax
from jax.experimental import pallas as pl
from jax.experimental.pallas import tpu as pltpu
from jax.sharding import PartitionSpec as P


GROUP_DIM = 128


EPSILON = 1e-06
REACH = 15
MESH = pl.DeviceIdType.MESH
PAIR = 2


def shifted(value, axis, steps):
    count = lax.axis_size(axis)
    initial, last = (max(0, -steps), min(count, count - steps))
    return lax.ppermute(value, axis, [(source, source + steps) for source in range(initial, last)])


def normalize(values, weight_gain):
    wide = values.astype(jnp.float32)
    factor = lax.rsqrt(jnp.mean(wide * wide, axis=-1, keepdims=True) + EPSILON)
    return (wide * factor * weight_gain).astype(jnp.bfloat16)


def swap(value, axis, mask):
    count = lax.axis_size(axis)
    return lax.ppermute(value, axis, [(source, source ^ mask) for source in range(count)])


def from_core(value):
    return swap(value, "tp", 1)


def from_chip(value, steps):
    count = lax.axis_size("tp")
    return lax.ppermute(
        value, "tp", [(source, (source + steps * PAIR) % count) for source in range(count)]
    )


def from_mate(value):
    return swap(value, "fs", PAIR)


def from_lane(value):
    return swap(value, "fs", 1)


def send_order(lines):
    return [1] + sorted(range(2, lines), reverse=True)


def fetch_halves(half, lanes=True):
    count = lax.axis_size("fs")
    lines = count // PAIR
    me = lax.axis_index("fs")
    line, lane = me // PAIR, me % PAIR
    own, other = half(line % PAIR), half(1 - line % PAIR)
    blocks = {0: own}
    for steps in send_order(lines):
        blocks[steps] = swap(other if steps % 2 else own, "fs", steps * PAIR)
    if not lanes:
        return list(blocks.values())
    found = []
    for steps, block in blocks.items():
        partner = from_lane(block)
        at = (line ^ steps) * PAIR
        found += [(block, at + lane), (partner, at + 1 - lane)]
    return found


def join(found, axis, place=lambda at: at):
    first = found[0][0]
    step = first.shape[axis]
    shape = list(first.shape)
    shape[axis] = step * len(found)
    full = jnp.zeros(shape, first.dtype)
    for block, at in found:
        start = [0] * len(shape)
        start[axis] = place(at) * step
        full = lax.dynamic_update_slice(full, block, start)
    return full


def fetch_pair(gate, upward):
    width = gate.shape[1] // PAIR

    def half(parity):
        parts = [lax.dynamic_slice_in_dim(w, parity * width, width, 1) for w in (gate, upward)]
        return jnp.concatenate(parts, 1)

    return fetch_halves(half)


def fetch_down(down, lanes=True):
    depth = down.shape[0] // PAIR
    return fetch_halves(
        lambda parity: lax.dynamic_slice_in_dim(down, parity * depth, depth, 0), lanes
    )


def fetch_mixer(mix_input, mix_output):
    both = jnp.stack([mix_input, mix_output.T])
    count = lax.axis_size("fs")
    lines = count // PAIR
    me = lax.axis_index("fs")
    line, lane = me // PAIR, me % PAIR
    found = [(both, line)]
    for steps in send_order(lines):
        found.append((swap(both, "fs", steps * PAIR), line ^ steps))
    block = stack_rows(found)
    partner = from_lane(block)
    depth, width = mix_input.shape
    tp = lax.axis_size("tp")
    pieces = [(v, lane, at) for v, at in gather_tp(block)]
    pieces += [(v, 1 - lane, at) for v, at in gather_tp(partner)]
    full = [jnp.zeros((lines, PAIR, depth, tp * width), both.dtype) for _ in range(2)]
    for value, at_lane, at in pieces:
        for which in range(2):
            piece = value[which].reshape(lines, 1, depth, width)
            full[which] = lax.dynamic_update_slice(full[which], piece, (0, at_lane, 0, at * width))
    return [value.reshape(count * depth, tp * width) for value in full]


def gather_tp(value):
    count = lax.axis_size("tp")
    chips = count // PAIR
    me = lax.axis_index("tp")
    chip, core = me // PAIR, me % PAIR
    found = []
    for steps in range(chips):
        if steps:
            block = from_chip(value, steps)
        else:
            block = value
        partner = from_core(block)
        place = (chip - steps + chips) % chips * PAIR
        found += [(block, place + core), (partner, place + 1 - core)]
    return found


def wide(value):
    return value.astype(jnp.float32)


def narrow(value):
    return value.astype(jnp.bfloat16)


def call(body, places, grid, operands, specs, out, out_spec, scratch, flops):
    moved = sum(value.size * value.dtype.itemsize for value in (*operands, out))
    spec = pltpu.PrefetchScalarGridSpec(
        num_scalar_prefetch=1,
        grid=grid,
        in_specs=specs,
        out_specs=out_spec,
        scratch_shapes=scratch,
    )
    return pl.pallas_call(
        body,
        out_shape=out,
        grid_spec=spec,
        cost_estimate=pl.CostEstimate(flops=flops, bytes_accessed=moved, transcendentals=0),
        compiler_params=pltpu.CompilerParams(vmem_limit_bytes=44 * 2**20),
    )(places, *operands)


def whole(value):
    return pl.BlockSpec(value.shape, lambda i, at: (0,) * len(value.shape))


def tile_of(size, limit):
    while size % limit:
        limit //= 2
    return limit


def stack_rows(found):
    blocks = [block for block, _ in found]
    count = len(blocks)
    *lead, depth, width = blocks[0].shape

    def body(at, *refs):
        for which in range(count):
            start = pl.multiple_of(at[which] * depth, depth)
            refs[-1][..., pl.ds(start, depth), :] = refs[which][...]

    out = jax.ShapeDtypeStruct((*lead, depth * count, width), blocks[0].dtype)
    places = jnp.stack([at for _, at in found]).astype(jnp.int32)
    specs = [whole(block) for block in blocks]
    return call(body, places, (1,), blocks, specs, out, whole(out), [], 0)


def hidden_units(parts, gain, pairs):
    blocks = [block for block, _ in pairs]
    places = jnp.stack([at for _, at in pairs]).astype(jnp.int32)
    depth = blocks[0].shape[0]
    rows, features = parts[0].shape
    units = blocks[0].shape[1] // 2
    tile, chunk = tile_of(rows, 512), tile_of(units, 256)
    tiles, several = rows // tile, len(parts)

    def body(at, *refs):
        values, gains, weights = refs[:several], refs[several], refs[several + 1 : -3]
        out, full, normed = refs[-3:]
        step = pl.program_id(0)

        @pl.when(step == 0)
        def _():
            for which, weight in enumerate(weights):
                start = pl.multiple_of(at[which] * depth, depth)
                full[pl.ds(start, depth), :] = weight[...]

        for which, value in enumerate(values):

            @pl.when(step // tiles == which)
            def _(value=value):
                normed[...] = normalize(value[...], gains[...])

        for start in range(0, units, chunk):
            gated, raised = [
                jnp.dot(
                    normed[...],
                    full[:, first + start : first + start + chunk],
                    preferred_element_type=jnp.float32,
                )
                for first in (0, units)
            ]
            value = gated / (1.0 + jnp.exp(-gated)) * raised
            out[:, start : start + chunk] = value.astype(out.dtype)

    def rows_of(which):
        return pl.BlockSpec(
            (tile, features), lambda i, at: (jnp.clip(i - which * tiles, 0, tiles - 1), 0)
        )

    gain = gain.reshape(1, features)
    return call(
        body,
        places,
        (several * tiles,),
        (*parts, gain, *blocks),
        [rows_of(which) for which in range(several)] + [whole(gain)] + [whole(w) for w in blocks],
        jax.ShapeDtypeStruct((several * rows, units), jnp.bfloat16),
        pl.BlockSpec((tile, units), lambda i, at: (i, 0)),
        [
            pltpu.VMEM((features, units * 2), jnp.bfloat16),
            pltpu.VMEM((tile, features), jnp.bfloat16),
        ],
        4 * several * rows * features * units,
    )


def down_rows(hidden, found, picked, arrived):
    blocks = [block for block, _ in found]
    count, width = len(blocks), blocks[0].shape[1]
    places = jnp.concatenate([jnp.stack([at for _, at in found]), picked]).astype(jnp.int32)
    _, run, units = hidden.shape
    groups = picked.shape[0]
    extra = [] if arrived is None else [arrived]

    def body(at, x, *refs):
        weights, out = refs[:count], refs[-1]
        for which, weight in enumerate(weights):
            columns = pl.ds(pl.multiple_of(at[which] * width, width), width)
            value = jnp.dot(x[0], weight[...], preferred_element_type=jnp.float32)
            if extra:
                value = value + refs[count][0, :, columns].astype(jnp.float32)
            out[0, :, columns] = value.astype(out.dtype)

    out = jax.ShapeDtypeStruct((groups, run, width * count), jnp.bfloat16)
    block = pl.BlockSpec((1, run, width * count), lambda i, at: (i, 0, 0))
    return call(
        body,
        places,
        (groups,),
        (hidden, *blocks, *extra),
        [pl.BlockSpec((1, run, units), lambda i, at: (at[count + i], 0, 0))]
        + [whole(w) for w in blocks]
        + [block] * len(extra),
        out,
        block,
        [],
        2 * groups * run * units * width * count,
    )


def flip(value, mask):
    bit = 1
    while bit <= mask:
        if mask & bit:
            value = value + bit - 2 * bit * ((value // bit) % 2)
        bit *= 2
    return value


def last_block(mid_run, gain, pairs, found, tokens_shape):
    tp, lines = lax.axis_size("tp"), lax.axis_size("fs") // PAIR
    chips, count = tp // PAIR, len(pairs)
    run, features = mid_run.shape
    row_count, width = tokens_shape
    ratio = count // tp
    g_blocks, d_blocks = [b for b, _ in pairs], found
    depth, units = g_blocks[0].shape[0], g_blocks[0].shape[1] // 2
    step, tile, chunk = d_blocks[0].shape[1], run * PAIR, tile_of(units, 256)
    upper, half = chips // 2, run // 2
    steps_of = [0] + send_order(lines)

    def body(mid, gains, *refs):
        gates, refs = refs[:count], refs[count:]
        downs, out = refs[:lines], refs[lines]
        rows, full, down, normed, hidden, sums, core_in = refs[lines + 1 : lines + 8]
        x_in, za_out, za_in, zb_in, xb_in, local, sent, landed = refs[lines + 8 :]
        fs, me = lax.axis_index("fs"), lax.axis_index("tp")
        line, lane = fs // PAIR, fs % PAIR
        chip, core = me // PAIR, me % PAIR
        away = {"tp": chip * PAIR + 1 - core}
        mate = {"fs": flip(line, 1) * PAIR + lane}
        across = {"fs": line * PAIR + 1 - lane}

        def chip_at(k):
            return (chip + k) % chips

        def chip_id(k):
            return {"tp": chip_at(k) * PAIR + core}

        peers = [away, across, mate] + [chip_id(k) for k in range(1, chips)]
        barrier = pltpu.get_barrier_semaphore()
        for peer in peers:
            pl.semaphore_signal(barrier, inc=1, device_id=peer, device_id_type=MESH)
        pl.semaphore_wait(barrier, len(peers))

        def copy(src, dst, at, peer):
            return pltpu.make_async_remote_copy(
                src_ref=src,
                dst_ref=dst,
                send_sem=sent.at[at],
                recv_sem=landed.at[at],
                device_id=peer,
                device_id_type=MESH,
            )

        numbers = iter(range(1000))
        started = []

        def send(src, dst, peer):
            made = copy(src, dst, next(numbers), peer)
            made.start()
            started.append(made)
            return made

        def place(which):
            found_lane = lane if which % PAIR == 0 else 1 - lane
            return flip(line, steps_of[which // PAIR]) * PAIR + found_lane

        to_core = send(mid, rows.at[0, me], away)
        to_chip = [send(mid, rows.at[0, me], chip_id(k)) for k in range(1, chips)]
        to_mate = send(mid, rows.at[1, me], mate)
        loads = [pltpu.make_async_copy(mid, rows.at[0, me], local.at[0])]
        for which in range(count):
            at = pl.ds(pl.multiple_of(place(which) * depth, depth), depth)
            loads.append(pltpu.make_async_copy(gates[which], full.at[at], local.at[1 + which]))
        for which in range(lines):
            loads.append(
                pltpu.make_async_copy(
                    downs[which], down.at[PAIR * which], local.at[1 + count + which]
                )
            )
        for load in loads:
            load.start()
        lanes_in = [
            send(downs[which], down.at[PAIR * which + 1], across) for which in range(lines)
        ]
        for load in loads:
            load.wait()

        def hide(side, at):
            values = rows[side, pl.ds(at * PAIR, PAIR)].reshape(tile, features)
            normed[...] = normalize(values, gains[...])
            for start in range(0, units, chunk):
                gated, raised = [
                    jnp.dot(
                        normed[...],
                        full[:, first + start : first + start + chunk],
                        preferred_element_type=jnp.float32,
                    )
                    for first in (0, units)
                ]
                value = gated / (1.0 + jnp.exp(-gated)) * raised
                hidden[side, at, :, start : start + chunk] = value.astype(hidden.dtype)

        def multiply(side, at):
            for which in range(count):
                target, piece = place(which) // ratio, place(which) % ratio
                ours = 1 - (target + core) % PAIR
                columns = pl.ds(pl.multiple_of(piece * step, step), step)
                value = jnp.dot(
                    hidden[side, at], down[which], preferred_element_type=jnp.float32
                )
                sums[ours, side, at, target // PAIR, :, columns] = value.astype(sums.dtype)
            return send(sums.at[0, side, at], core_in.at[side, at], away)

        base = 100

        def x_first(side, at):
            return [
                copy(
                    sums.at[1, side, at, chip_at(k)],
                    x_in.at[side, at, k - 1],
                    base + (side * chips + at) * chips + k,
                    chip_id(k),
                )
                for k in range(1, chips)
            ]

        def z_first(at):
            return copy(
                sums.at[1, 1, at], zb_in.at[at], base + 2 * chips * chips + at, mate
            )

        def merge(side, at, exchange):
            exchange.wait_recv()
            total = wide(sums[1, side, at]) + wide(core_in[side, at])
            sums[1, side, at] = narrow(total)

            @pl.when(at < upper)
            def _():
                for made in x_first(side, at):
                    made.start()

            if side:

                @pl.when(at >= upper)
                def _():
                    z_first(at).start()

        tiles = [chip] + [chip_at(chips - k) for k in range(1, chips)]

        def run_at(k):
            return chip_at(chips - k) * PAIR + core

        to_core.wait_recv()
        hide(0, chip)
        passed = []
        for k in range(1, chips):
            to_chip[k - 1].wait_recv()
            block = rows.at[0, run_at(k)]
            passed.append(send(block, rows.at[0, run_at(k)], away))
        to_mate.wait_recv()
        mate_passed = send(rows.at[1, me], rows.at[1, me], away)
        first_half, second_half = pl.ds(0, half), pl.ds(half, half)
        halves = []
        for k in range(1, chips):
            halves.append(
                (
                    send(
                        rows.at[1, me, first_half], rows.at[1, me, first_half], chip_id(k)
                    ),
                    send(
                        rows.at[0, run_at(k), second_half],
                        rows.at[1, run_at(k), second_half],
                        mate,
                    ),
                )
            )
        for k in range(1, chips):
            passed[k - 1].wait_recv()
            hide(0, tiles[k])
        mate_passed.wait_recv()
        hide(1, chip)
        diagonal = []
        for k in range(1, chips):
            for made, part in zip(halves[k - 1], (first_half, second_half)):
                made.wait_recv()
                block = rows.at[1, run_at(k), part]
                diagonal.append(send(block, rows.at[1, run_at(k), part], away))
        for made in lanes_in:
            made.wait_recv()
        ready = [(0, chip)] + [(0, tiles[k]) for k in range(1, chips)] + [(1, chip)]
        last = None
        for side, at in ready:
            exchange = multiply(side, at)
            if last is not None:
                merge(*last)
            last = (side, at, exchange)
        for k in range(1, chips):
            for made in diagonal[2 * k - 2 : 2 * k]:
                made.wait_recv()
            hide(1, tiles[k])
            merge(*last)
            last = (1, tiles[k], multiply(1, tiles[k]))
        merge(*last)

        def arrived_x(side, at, total):
            for k in range(1, chips):
                x_first(side, at)[k - 1].wait_recv()
                total = total + wide(x_in[side, at, k - 1])
            return total

        def second_x(at):
            return [
                copy(
                    sums.at[1, 0, at, chip_at(k)],
                    xb_in.at[at, k - 1],
                    base + 2 * chips * chips + (2 + k) * chips + at,
                    chip_id(k),
                )
                for k in range(1, chips)
            ]

        def second_z(at):
            return copy(
                za_out.at[at], za_in.at[at], base + 2 * chips * chips + chips + at, mate
            )

        def finish(at, total):
            kept = rows[
                0,
                at * PAIR : (at + 1) * PAIR,
                :,
                pl.ds(pl.multiple_of(me * width, width), width),
            ].reshape(tile, width)
            out[at * tile : (at + 1) * tile, :] = narrow(wide(kept) + 0.5 * total)

        for at in range(upper):
            za_out[at] = narrow(arrived_x(1, at, wide(sums[1, 1, at, chip])))
            second_z(at).start()
        for at in range(upper, chips):
            z_first(at).wait_recv()
            sums[1, 0, at] = narrow(wide(sums[1, 0, at]) + wide(zb_in[at]))
            for made in second_x(at):
                made.start()
        for at in range(upper):
            total = arrived_x(0, at, wide(sums[1, 0, at, chip]))
            second_z(at).wait_recv()
            finish(at, total + wide(za_in[at]))
        for at in range(upper, chips):
            total = wide(sums[1, 0, at, chip])
            for k, made in enumerate(second_x(at)):
                made.wait_recv()
                total = total + wide(xb_in[at, k])
            finish(at, total)
        for made in started:
            made.wait_send()
        for at in range(chips):
            if at < upper:
                for made in x_first(0, at) + x_first(1, at) + [second_z(at)]:
                    made.wait_send()
            else:
                for made in [z_first(at)] + second_x(at):
                    made.wait_send()

    bf16 = jnp.bfloat16
    total = 100 + 2 * chips * chips + (3 + chips) * chips
    gain = gain.reshape(1, features)
    any_space = pl.BlockSpec(memory_space=pl.ANY)
    in_vmem = pl.BlockSpec(memory_space=pltpu.VMEM)
    return pl.pallas_call(
        body,
        out_shape=jax.ShapeDtypeStruct((row_count, width), bf16),
        in_specs=[any_space, in_vmem] + [any_space] * (count + lines),
        out_specs=in_vmem,
        scratch_shapes=[
            pltpu.VMEM((2, tp, run, features), bf16),
            pltpu.VMEM((features, 2 * units), bf16),
            pltpu.VMEM((count, units, step), bf16),
            pltpu.VMEM((tile, features), bf16),
            pltpu.VMEM((2, chips, tile, units), bf16),
            pltpu.VMEM((2, 2, chips, chips, tile, width), bf16),
            pltpu.VMEM((2, chips, chips, tile, width), bf16),
            pltpu.VMEM((2, chips, chips - 1, tile, width), bf16),
            pltpu.VMEM((chips, tile, width), bf16),
            pltpu.VMEM((chips, tile, width), bf16),
            pltpu.VMEM((chips, chips, tile, width), bf16),
            pltpu.VMEM((chips, chips - 1, tile, width), bf16),
            pltpu.SemaphoreType.DMA((1 + count + lines,)),
            pltpu.SemaphoreType.DMA((total,)),
            pltpu.SemaphoreType.DMA((total,)),
        ],
        name="last",
        compiler_params=pltpu.CompilerParams(
            collective_id=0, has_side_effects=True, vmem_limit_bytes=58 * 2**20
        ),
    )(mid_run, gain, *g_blocks, *d_blocks)


def send_x(part):
    chips = lax.axis_size("tp") // PAIR
    chip = lax.axis_index("tp") // PAIR
    total = wide(part(chip))
    for steps in range(1, chips):
        sent = part((chip + steps) % chips)
        total = total + wide(from_chip(sent, steps))
    return total


def scatter(one, two):
    chips = lax.axis_size("tp") // PAIR
    mine, theirs = [send_x(lambda c: one(which, c)) for which in range(2)]
    arrived = from_mate(jnp.stack([two(1, c) for c in range(chips)]))
    own = jnp.stack([two(0, c) for c in range(chips)])
    merged = narrow(wide(own) + wide(arrived))
    arrived = from_mate(narrow(theirs))
    first = wide(narrow(mine)) + wide(arrived)
    second = send_x(lambda c: lax.dynamic_index_in_dim(merged, c, 0, keepdims=False))
    return first, second


def pool_groups(extended, positions, pool_weight, pool_scale):
    row_count = positions.shape[0]
    group_count = extended.shape[1] // GROUP_DIM
    group_ids = jnp.arange(group_count, dtype=jnp.int32)
    windows = jnp.left_shift(2, group_ids % 4)
    window_cols = jnp.repeat(windows, GROUP_DIM)[None, :]
    values = wide(extended)
    summed = jnp.zeros((row_count, values.shape[1]), jnp.float32)
    for offset in range(REACH + 1):
        moved = values[REACH - offset : REACH - offset + row_count]
        summed = summed + jnp.where(offset < window_cols, moved, 0.0)
    counts = jnp.minimum(positions[:, None] + 1, window_cols).astype(jnp.float32)
    pooled = narrow(summed / counts - values[REACH:])
    mapped = jnp.einsum(
        "tgc,gcd->tgd",
        pooled.reshape(row_count, group_count, GROUP_DIM),
        pool_weight,
        preferred_element_type=jnp.float32,
    )
    return narrow(mapped.reshape(row_count, group_count * GROUP_DIM) * pool_scale)


def per_device(
    tokens,
    first_gain,
    first_gate,
    first_upward,
    first_down,
    mix_gain,
    mix_input,
    pool_weight,
    pool_scale,
    mix_output,
    second_gain,
    second_gate,
    second_upward,
    second_down,
):
    tp = lax.axis_size("tp")
    chips = tp // PAIR
    me = lax.axis_index("tp")
    core = me % PAIR
    row_count, width = tokens.shape
    run = row_count // tp
    depth = width * tp

    mate_tokens = from_mate(tokens)
    own_rows = join(gather_tp(tokens), 1)
    mate_rows = join(gather_tp(mate_tokens), 1)

    pairs_1 = fetch_pair(first_gate, first_upward)
    down_1 = fetch_down(first_down)
    pairs_2 = fetch_pair(second_gate, second_upward)
    down_2 = fetch_down(second_down, lanes=False)
    full_input, full_output = fetch_mixer(mix_input, mix_output)

    hidden = hidden_units((own_rows, mate_rows), first_gain, pairs_1)
    runs = hidden.reshape(2 * tp, run, hidden.shape[1])

    def groups(which):
        return jnp.stack([s * tp + c * PAIR + which for s in range(2) for c in range(chips)])

    sent = down_rows(runs, down_1, groups(1 - core), None)
    arrived = from_core(sent)
    sums = down_rows(runs, down_1, groups(core), arrived)
    sums = sums.reshape(2, chips, run, depth)

    def columns(first, last):
        return lambda s, c: lax.dynamic_slice(
            sums, (s, c, 0, first), (1, 1, run, last - first)
        ).reshape(run, last - first)

    half = depth // 2
    summed = jnp.concatenate(scatter(columns(0, half), columns(half, depth)), 1)
    own_run = lax.dynamic_slice_in_dim(own_rows, me * run, run, 0)
    first_out = narrow(wide(own_run) + 0.5 * summed)

    normed = normalize(first_out, mix_gain)
    pool_in = narrow(jnp.dot(normed, full_input, preferred_element_type=jnp.float32))
    prior = shifted(pool_in[run - REACH :], "tp", 1)
    extended = jnp.concatenate([prior, pool_in], 0)
    positions = me * run + jnp.arange(run, dtype=jnp.int32)
    mapped = pool_groups(extended, positions, pool_weight, pool_scale)
    mixed = lax.dot_general(
        mapped, full_output, (((1,), (1,)), ((), ())), preferred_element_type=jnp.float32
    )
    mid_run = narrow(wide(first_out) + mixed)

    return last_block(mid_run, second_gain, pairs_2, down_2, tokens.shape)


def solution(mesh):
    in_specs = (
        P("fs", "tp"),
        P(),
        P("fs", "tp"),
        P("fs", "tp"),
        P("tp", "fs"),
        P(),
        P("fs", "tp"),
        P(),
        P(),
        P("tp", "fs"),
        P(),
        P("fs", "tp"),
        P("fs", "tp"),
        P("tp", "fs"),
    )
    out_specs = P("fs", "tp")
    return jax.shard_map(
        per_device, mesh=mesh, in_specs=in_specs, out_specs=out_specs, check_vma=False
    )
```
